32 devices in a mesh: vp: 8 (over z, x), dp: 4 (over y, core).
Axes of the slice: x: 2, y: 2, z: 4, core: 2. Of those that a mesh axis runs over, the one named last changes fastest.
Arguments:
- hidden: bfloat16 [4096, 5632], P(('vp', 'dp')), may hold values from -6 to 6
- down_weight: bfloat16 [5632, 2048], P('vp'), may hold values from -0.078125 to 0.078125
- residual: bfloat16 [4096, 2048], P(('vp', 'dp')), may hold values from -20 to 20
- post_gain: float32 [2048], replicated, may hold values from 0.1 to 1.9
- final_gain: float32 [2048], replicated, may hold values from 0.1 to 1.9
- vocab_matrix: bfloat16 [2048, 32768], P(None, 'vp'), may hold values from -8 to 8
- vocab_bias: float32 [32768], P('vp'), may hold values from -3.5 to 3.5
- targets: int32 [4096], P(('vp', 'dp')), may hold values from 0 to 32767
Outputs:
- losses: float32 [4096], P(('vp', 'dp'))
- norm_grad: float32 [4096, 2048], P(('vp', 'dp'))
- vocab_grad: float32 [2048, 32768], P('dp', 'vp')
The draws below stay inside these ranges and needn't reach their ends.
All inputs are finite; a program needn't handle non-finite values.
Results may differ from the reference program's by a relative error of at most 0.01.
Values may be sent and summed in bfloat16 or wider, within the bound.
A program may use at most 128 MiB of HBM per device.

```python
import math
import jax
import jax.numpy as jnp
import numpy as np
from jax import lax

D = 2048
FF = 5632
VOCAB = 32768
TOKENS = 4096
N_VP = 8


def draw_vocab_matrix(key, part):
    drawn_key = jax.random.fold_in(jax.random.fold_in(key, 11), 0)
    spread = (D // 6) ** (-0.5)
    matrix = jnp.clip(jax.random.normal(drawn_key, (D, VOCAB), jnp.float32), -6.0, 6.0) * spread
    return matrix.astype(jnp.bfloat16)


def draw_residual(key, part):
    base_key = jax.random.fold_in(jax.random.fold_in(key, 22), 1)
    values = jnp.clip(jax.random.normal(base_key, (TOKENS, D), jnp.float32), -6.0, 6.0)
    return values.astype(jnp.bfloat16)


def draw_vocab_bias(key, part):
    column_ids = jnp.arange(VOCAB)
    shard_ids = (column_ids // (VOCAB // N_VP)).astype(jnp.float32)
    shifted = 3.0 * shard_ids / max(N_VP - 1, 1) - 1.5
    jitter = jnp.clip(0.7 * jax.random.normal(key, (VOCAB,), jnp.float32), -2.0, 2.0)
    return (shifted + jitter).astype(jnp.float32)


def with_ends(result, key, smallest, high):
    longest = result.shape.index(max(result.shape))
    spots = []
    for shift in (0, 1):
        where = [jax.random.randint(jax.random.fold_in(key, axis), (), 0, length) for axis, length in enumerate(result.shape)]
        where[longest] = (where[longest] + shift) % result.shape[longest]
        spots.append(tuple(where))
    return result.at[spots[0]].set(smallest).at[spots[1]].set(high)


def block_scale(stream_key, dims, pieces, low, top_value):
    def one(dim, parts):
        heights = jax.random.uniform(jax.random.fold_in(jax.random.fold_in(stream_key, 6), dim), (parts,), jnp.float32, low / len(pieces), top_value / len(pieces))
        return jnp.repeat(jnp.exp(heights), dims[dim] // parts).reshape((-1,) + (1,) * (len(dims) - dim - 1))

    level = one(*pieces[0])
    for cut in pieces[1:]:
        level = level * one(*cut)
    return level


def cumulative_ranks(number_of, lean):
    portions = [(1 << 20) // math.isqrt(rank ** lean) + 1 for rank in range(1, number_of + 1)]
    scale = 1 + sum(portions) // (1 << 30)
    return np.cumsum(np.array([max(1, weight // scale) for weight in portions]))


def ranked_ids(own_key, dims, amount, lean):
    grid = cumulative_ranks(amount, lean)
    pick = jax.random.randint(jax.random.fold_in(own_key, 1), dims, 0, int(grid[amount - 1]))
    rank = jnp.searchsorted(jnp.asarray(grid, jnp.int32), pick, side="right")
    return jax.random.permutation(jax.random.fold_in(own_key, 2), amount)[rank].astype(jnp.int32)


def normal_values(rng, dims, scale, reach, cuts=(), kind=jnp.bfloat16):
    result = jax.random.normal(rng, dims, jnp.float32) * scale
    if len(cuts) > 0:
        result = block_scale(rng, dims, cuts, -0.22, 0.18) * result
    return jnp.clip(result, min=-reach, max=reach).astype(kind)


def setup_inputs(seed: int = 0) -> dict:
    streams_of = jax.random.split(jax.random.key(seed), 9)
    return {
        "hidden": normal_values(streams_of[0], (TOKENS, FF), 1.0, 6.0, ((0, 32),)),
        "down_weight": normal_values(streams_of[1], (FF, D), FF ** -0.5, 0.078125, ((0, 8),)),
        "residual": draw_residual(jax.random.fold_in(streams_of[8], 71), 0),
        "post_gain": jnp.clip(1.0 + 0.18 * jax.random.normal(streams_of[3], (D,), jnp.float32), 0.1, 1.9),
        "final_gain": jnp.clip(1.0 + 0.18 * jax.random.normal(streams_of[4], (D,), jnp.float32), 0.1, 1.9),
        "vocab_matrix": draw_vocab_matrix(jax.random.fold_in(streams_of[8], 71), 0),
        "vocab_bias": draw_vocab_bias(jax.random.fold_in(streams_of[8], 71), 0),
        "targets": with_ends(ranked_ids(streams_of[7], (TOKENS,), VOCAB, 2), jax.random.fold_in(streams_of[7], 3), 0, VOCAB - 1).astype(jnp.int32),
    }


norm_eps = 1e-06
zloss_weight = 0.0001

def reference(hidden, down_weight, residual, post_gain, final_gain, vocab_matrix, vocab_bias, targets):
    mixed_rows = jnp.dot(hidden, down_weight, preferred_element_type=jnp.float32)
    post_scaled = mixed_rows * lax.rsqrt(lax.optimization_barrier(jnp.mean(mixed_rows * mixed_rows, axis=-1, keepdims=True)) + norm_eps)
    stream = (residual.astype(jnp.float32) + post_scaled * post_gain[None, :]).astype(jnp.bfloat16)
    stream_f = stream.astype(jnp.float32)
    inverse = lax.rsqrt(lax.optimization_barrier(jnp.mean(stream_f * stream_f, axis=-1, keepdims=True)) + norm_eps)
    scaled = stream_f * inverse
    normed = (scaled * final_gain[None, :]).astype(jnp.bfloat16)
    total_rows = normed.shape[0]
    block_rows = math.gcd(total_rows, 512)
    block_count = total_rows // block_rows
    column_ids = lax.broadcasted_iota(jnp.int32, (1, vocab_matrix.shape[1]), 1)

    def one_block(grad_state, inputs):
        normed_block, target_block = inputs
        logits = jnp.dot(normed_block, vocab_matrix, preferred_element_type=jnp.float32) + vocab_bias[None, :]
        row_max = lax.optimization_barrier(jnp.max(logits, axis=1))
        log_total = row_max + jnp.log(lax.optimization_barrier(jnp.sum(jnp.exp(logits - row_max[:, None]), axis=1)))
        hit_mask = column_ids == target_block[:, None]
        picked = lax.optimization_barrier(jnp.sum(jnp.where(hit_mask, logits, 0.0), axis=1))
        block_loss = log_total - picked + zloss_weight * log_total * log_total
        grad_scale = 1.0 + 2.0 * zloss_weight * log_total
        dlogits = (jnp.exp(logits - log_total[:, None]) * grad_scale[:, None] - jnp.where(hit_mask, 1.0, 0.0)).astype(jnp.bfloat16)
        dnormed = lax.dot_general(dlogits, vocab_matrix, (((1,), (1,)), ((), ())), preferred_element_type=jnp.float32)
        grad_state = grad_state + lax.dot_general(normed_block, dlogits, (((0,), (0,)), ((), ())), preferred_element_type=jnp.float32)
        return (grad_state, (block_loss, dnormed))
    start_grad = jnp.zeros(vocab_matrix.shape, jnp.float32)
    vocab_grad, outputs = lax.scan(one_block, start_grad, (normed.reshape(block_count, block_rows, -1), targets.reshape(block_count, block_rows)))
    losses = outputs[0].reshape(total_rows)
    dnormed = outputs[1].reshape(total_rows, -1)
    dscaled = dnormed * final_gain[None, :]
    norm_grad = inverse * (dscaled - scaled * lax.optimization_barrier(jnp.mean(dscaled * scaled, axis=-1, keepdims=True)))
    return (losses, norm_grad, vocab_grad)
```

```python
import functools
import math

import jax
import jax.numpy as jnp
from jax import lax
from jax.experimental import pallas as pl
from jax.experimental.pallas import tpu as pltpu
from jax.sharding import PartitionSpec as P

norm_eps = 1e-06
zloss_weight = 0.0001
MESH = pl.DeviceIdType.MESH
f32, bf16 = jnp.float32, jnp.bfloat16


class Place:
    def __init__(self, nx, nz):
        self.nx, self.nz, self.count = nx, nz, nx * nz
        self.vp, self.dp = lax.axis_index("vp"), lax.axis_index("dp")
        self.x, self.z = lax.rem(self.vp, nx), self.vp // nx
        self.other_core = self.dp + 1 - 2 * lax.rem(self.dp, 2)

    def side(self, step):
        return lax.rem(self.x + step, self.nx)

    def at(self, x, z):
        return (z * self.nx + x, self.dp)

    def outward(self, k):
        return jnp.where(lax.rem(k, 2) == 0, k // 2, self.nz - 1 - k // 2)

    def nearby(self, k):
        low, high = self.z, self.nz - 1 - self.z
        both = jnp.minimum(low, high)
        half = (k + 1) // 2
        near = jnp.where(lax.rem(k, 2) == 1, self.z - half, self.z + half)
        far = jnp.where(high > low, self.z + (k - both), self.z - (k - both))
        return jnp.where(k <= 2 * both, near, far)


def arrived(ref, sem):
    pltpu.make_async_copy(ref, ref, sem).wait()


def send(src, dst, send_sem, recv_sem, device):
    pltpu.make_async_remote_copy(
        src_ref=src, dst_ref=dst, send_sem=send_sem, recv_sem=recv_sem,
        device_id=device, device_id_type=MESH,
    ).start()


def greet(place, everyone):
    barrier = pltpu.get_barrier_semaphore()
    for step in range(1, place.count):
        peer = lax.rem(place.vp + step, place.count)
        pl.semaphore_signal(barrier, inc=1, device_id=(peer, place.dp), device_id_type=MESH)
        if everyone:
            pl.semaphore_signal(
                barrier, inc=1, device_id=(peer, place.other_core), device_id_type=MESH
            )
    pl.semaphore_signal(
        barrier, inc=1, device_id=(place.vp, place.other_core), device_id_type=MESH
    )
    pl.semaphore_wait(barrier, place.count + (place.count - 1 if everyone else 0))


def row_loop(rows, size, body):
    @pl.loop(0, rows // size)
    def _(r):
        body(pl.ds(pl.multiple_of(r * size, size), size))


def line_reduce_scatter(place, splits, produce, px, xr, q, sb, zd, zu, sems):
    nx, nz, z = place.nx, place.nz, place.z
    xs_sem, xr_sem, zs_sem, zd_sem, zu_sem = sems
    rows = q.shape[2]
    size = min(rows, 32)

    def add(zb, s, ref):
        def body(r):
            q[zb, s, r] += ref[r].astype(f32)

        row_loop(rows, size, body)

    def pass_on(zb, s):
        def body(r):
            sb[zb, s, r] = q[zb, s, r].astype(bf16)

        row_loop(rows, size, body)

    def below(zb, s):
        @pl.when(z < nz - 1)
        def _():
            arrived(zd.at[zb, s], zd_sem.at[zb, s])
            add(zb, s, zd.at[zb, s])

    def above(zb, s):
        @pl.when(z > 0)
        def _():
            arrived(zu.at[zb, s], zu_sem.at[zb, s])
            add(zb, s, zu.at[zb, s])

    def sides(zb, s):
        for step in range(1, nx):
            arrived(xr.at[step - 1, zb, s], xr_sem.at[step - 1, zb, s])
            add(zb, s, xr.at[step - 1, zb, s])

    @pl.loop(0, nz + 1)
    def _(k):
        @pl.when(k < nz)
        def _():
            zb = place.outward(k)
            produce(zb)
            for s in range(splits):
                for step in range(1, nx):
                    slot = nx - step - 1
                    send(px.at[step - 1, zb, s], xr.at[slot, zb, s], xs_sem.at[step - 1, zb, s],
                         xr_sem.at[slot, zb, s], place.at(place.side(step), z))

        zc = place.outward(jnp.maximum(k - 1, 0))

        @pl.when((k > 0) & (zc < z))
        def _():
            for s in range(splits):
                sides(zc, s)
                below(zc, s)
                pass_on(zc, s)
                send(sb.at[zc, s], zd.at[zc, s], zs_sem.at[zc, s], zd_sem.at[zc, s],
                     place.at(place.x, z - 1))

        @pl.when((k > 0) & (zc > z))
        def _():
            for s in range(splits):
                sides(zc, s)
                above(zc, s)
                pass_on(zc, s)
                send(sb.at[zc, s], zu.at[zc, s], zs_sem.at[zc, s], zu_sem.at[zc, s],
                     place.at(place.x, z + 1))

    for s in range(splits):
        sides(z, s)
        below(z, s)
        above(z, s)

    @pl.loop(0, nz)
    def _(zb):
        for s in range(splits):
            for step in range(1, nx):
                arrived(px.at[step - 1, zb, s], xs_sem.at[step - 1, zb, s])

            @pl.when(zb != z)
            def _():
                arrived(sb.at[zb, s], zs_sem.at[zb, s])


def front_kernel(
    nx, nz, splits,
    hid, weight, residual, post_gain, final_gain, targets,
    normed_out, stream_out, targets_out,
    units, px, xr, q, sb, zd, zu, normed,
    xs_sem, xr_sem, zs_sem, zd_sem, zu_sem,
    hid_send, hid_recv, tgt_send, tgt_recv,
    side_send, line_send, gather_recv, core_send, core_recv, out_sem,
):
    place = Place(nx, nz)
    count, vp, z = place.count, place.vp, place.z
    split_rows, width = q.shape[2], q.shape[3]
    greet(place, True)

    own = pltpu.make_async_copy(hid.at[vp], units.at[vp], hid_recv.at[vp])
    own.start()
    for k in range(count - 1):
        peer = lax.rem(vp + k + 1, count)
        send(hid.at[peer], units.at[vp], hid_send.at[k], hid_recv.at[vp], (peer, place.dp))
    for k in range(count - 1):
        peer = lax.rem(vp + k + 1, count)
        for c in range(2):
            send(targets, targets_out.at[c, vp], tgt_send.at[c, k], tgt_recv.at[c, vp],
                 (peer, place.other_core if c else place.dp))
    send(targets, targets_out.at[1, vp], tgt_send.at[1, count - 1], tgt_recv.at[1, vp],
         (vp, place.other_core))
    own_targets = pltpu.make_async_copy(targets, targets_out.at[0, vp], tgt_recv.at[0, vp])
    own_targets.start()

    def product(device, store):
        arrived(units.at[device], hid_recv.at[device])
        tile = min(width, 512)

        @pl.loop(0, width // tile)
        def _(n):
            cols = pl.ds(pl.multiple_of(n * tile, tile), tile)
            store(cols, jnp.dot(units[device], weight[:, cols], preferred_element_type=f32))

    def produce(zb):
        for step in range(nx):
            def store(cols, value):
                for s in range(splits):
                    part = value[s * split_rows : (s + 1) * split_rows]
                    if step == 0:
                        q[zb, s, :, cols] = part
                    else:
                        px[step - 1, zb, s, :, cols] = part.astype(bf16)

            product(zb * nx + place.side(step), store)

    line_reduce_scatter(
        place, splits, produce, px, xr, q, sb, zd, zu, (xs_sem, xr_sem, zs_sem, zd_sem, zu_sem)
    )

    for s in range(splits):
        def norms(r):
            mixed = q[z, s, r]
            post = mixed * lax.rsqrt(jnp.mean(mixed * mixed, axis=-1, keepdims=True) + norm_eps)
            stream = (residual[s, r].astype(f32) + post * post_gain[...]).astype(bf16)
            stream_out[s, r] = stream
            stream = stream.astype(f32)
            inverse = lax.rsqrt(jnp.mean(stream * stream, axis=-1, keepdims=True) + norm_eps)
            normed[0, vp, s, r] = (stream * inverse * final_gain[...]).astype(bf16)

        row_loop(split_rows, 16, norms)

    def keep(c, i, s):
        pltpu.make_async_copy(normed.at[c, i, s], normed_out.at[c, i, s], out_sem.at[c, i, s]).start()

    def to_core(i, s):
        keep(0, i, s)
        send(normed.at[0, i, s], normed.at[1, i, s], core_send.at[i, s], core_recv.at[i, s],
             (vp, place.other_core))

    @pl.loop(0, nz + 1)
    def _(k):
        @pl.when(k < nz)
        def _():
            zb = place.nearby(k)
            i = zb * nx + place.x
            for s in range(splits):
                block, sem = normed.at[0, i, s], gather_recv.at[i, s]

                @pl.when(k > 0)
                def _():
                    arrived(block, sem)

                @pl.when((zb >= z) & (z > 0))
                def _():
                    send(block, block, line_send.at[0, zb, s], sem, place.at(place.x, z - 1))

                @pl.when((zb <= z) & (z < nz - 1))
                def _():
                    send(block, block, line_send.at[1, zb, s], sem, place.at(place.x, z + 1))

                for step in range(1, nx):
                    send(block, block, side_send.at[step - 1, zb, s], sem,
                         place.at(place.side(step), z))
                to_core(i, s)

        @pl.when(k > 0)
        def _():
            zb = place.nearby(k - 1)
            for step in range(1, nx):
                i = zb * nx + place.side(step)
                for s in range(splits):
                    arrived(normed.at[0, i, s], gather_recv.at[i, s])
                    to_core(i, s)

    @pl.loop(0, count)
    def _(i):
        for s in range(splits):
            arrived(normed.at[1, i, s], core_recv.at[i, s])
            keep(1, i, s)

    @pl.loop(0, nz)
    def _(zb):
        for s in range(splits):
            block = normed.at[0, zb * nx + place.x, s]

            @pl.when((zb >= z) & (z > 0))
            def _():
                arrived(block, line_send.at[0, zb, s])

            @pl.when((zb <= z) & (z < nz - 1))
            def _():
                arrived(block, line_send.at[1, zb, s])

            for step in range(1, nx):
                arrived(block, side_send.at[step - 1, zb, s])

    @pl.loop(0, count)
    def _(i):
        for c in range(2):
            arrived(targets_out.at[c, i], tgt_recv.at[c, i])
        for s in range(splits):
            arrived(normed.at[0, i, s], core_send.at[i, s])
            for c in range(2):
                arrived(normed.at[c, i, s], out_sem.at[c, i, s])

    for k in range(count - 1):
        arrived(hid.at[0], hid_send.at[k])
        for c in range(2):
            arrived(targets, tgt_send.at[c, k])
    arrived(targets, tgt_send.at[1, count - 1])


def rs_scratch(nx, nz, splits, rows, width):
    shape = (nz, splits, rows, width)
    return [
        pltpu.VMEM((nx - 1,) + shape, bf16),
        pltpu.VMEM((nx - 1,) + shape, bf16),
        pltpu.VMEM(shape, f32),
        pltpu.VMEM(shape, bf16),
        pltpu.VMEM(shape, bf16),
        pltpu.VMEM(shape, bf16),
    ]


def rs_sems(nx, nz, splits):
    dma = pltpu.SemaphoreType.DMA
    return [dma((nx - 1, nz, splits))] * 2 + [dma((nz, splits))] * 3


def front(nx, nz, splits, hid, weight, residual, post_gain, final_gain, targets):
    count, rows, _ = hid.shape
    width = weight.shape[1]
    split_rows = rows // splits
    dma = pltpu.SemaphoreType.DMA
    vmem = pl.BlockSpec(memory_space=pltpu.VMEM)
    flops = 2 * count * rows * weight.shape[0] * width
    return pl.pallas_call(
        functools.partial(front_kernel, nx, nz, splits),
        out_shape=(
            jax.ShapeDtypeStruct((2, count, splits, split_rows, width), bf16),
            jax.ShapeDtypeStruct((splits, split_rows, width), bf16),
            jax.ShapeDtypeStruct((2, count, 1, targets.shape[1]), jnp.int32),
        ),
        in_specs=[vmem] * 6,
        out_specs=(pl.BlockSpec(memory_space=pl.ANY), vmem, vmem),
        scratch_shapes=[pltpu.VMEM(hid.shape, bf16)]
        + rs_scratch(nx, nz, splits, split_rows, width)
        + [pltpu.VMEM((2, count, splits, split_rows, width), bf16)]
        + rs_sems(nx, nz, splits)
        + [
            dma((count - 1,)), dma((count,)), dma((2, count)), dma((2, count)),
            dma((nx - 1, nz, splits)), dma((2, nz, splits)), dma((count, splits)),
            dma((count, splits)), dma((count, splits)), dma((2, count, splits)),
        ],
        compiler_params=pltpu.CompilerParams(
            collective_id=0, has_side_effects=True, vmem_limit_bytes=60 << 20
        ),
        cost_estimate=pl.CostEstimate(flops=flops, bytes_accessed=1 << 24, transcendentals=0),
        name="front",
    )(hid, weight, residual.reshape(splits, split_rows, width), post_gain, final_gain, targets)


def back_kernel(
    nx, nz, splits,
    partial, own_out,
    mine, theirs, px, xr, q, sb, zd, zu,
    xs_sem, xr_sem, zs_sem, zd_sem, zu_sem,
    load_sem, core_send, core_recv,
):
    place = Place(nx, nz)
    count, z = place.count, place.z
    split_rows = q.shape[2]
    greet(place, False)

    @pl.loop(0, nz)
    def _(k):
        zb = place.outward(k)
        for step in range(nx):
            i = zb * nx + place.side(step)
            for s in range(splits):
                pltpu.make_async_copy(partial.at[0, i, s], mine.at[i, s], load_sem.at[i, s]).start()
                send(partial.at[1, i, s], theirs.at[i, s], core_send.at[i, s], core_recv.at[i, s],
                     (place.vp, place.other_core))

    def produce(zb):
        for step in range(nx):
            i = zb * nx + place.side(step)
            for s in range(splits):
                arrived(mine.at[i, s], load_sem.at[i, s])
                arrived(theirs.at[i, s], core_recv.at[i, s])

                def body(r):
                    value = mine[i, s, r].astype(f32) + theirs[i, s, r].astype(f32)
                    if step == 0:
                        q[zb, s, r] = value
                    else:
                        px[step - 1, zb, s, r] = value.astype(bf16)

                row_loop(split_rows, 16, body)

    line_reduce_scatter(
        place, splits, produce, px, xr, q, sb, zd, zu, (xs_sem, xr_sem, zs_sem, zd_sem, zu_sem)
    )
    for s in range(splits):
        def body(r):
            own_out[s, r] = q[z, s, r]

        row_loop(split_rows, 16, body)

    @pl.loop(0, count)
    def _(i):
        for s in range(splits):
            arrived(mine.at[i, s], core_send.at[i, s])


def back(nx, nz, splits, partial):
    _, count, _, split_rows, width = partial.shape
    dma = pltpu.SemaphoreType.DMA
    shape = (count, splits, split_rows, width)
    return pl.pallas_call(
        functools.partial(back_kernel, nx, nz, splits),
        out_shape=jax.ShapeDtypeStruct((splits, split_rows, width), f32),
        in_specs=[pl.BlockSpec(memory_space=pl.ANY)],
        out_specs=pl.BlockSpec(memory_space=pltpu.VMEM),
        scratch_shapes=[pltpu.VMEM(shape, bf16), pltpu.VMEM(shape, bf16)]
        + rs_scratch(nx, nz, splits, split_rows, width)
        + rs_sems(nx, nz, splits)
        + [dma((count, splits)), dma((count, splits)), dma((count, splits))],
        compiler_params=pltpu.CompilerParams(
            collective_id=1, has_side_effects=True, vmem_limit_bytes=40 << 20
        ),
        cost_estimate=pl.CostEstimate(flops=1 << 32, bytes_accessed=1 << 24, transcendentals=0),
        name="back",
    )(partial)


def combine(earlier, later):
    joined_max = jnp.maximum(earlier[0], later[0])
    joined_total = earlier[1] * jnp.exp(earlier[0] - joined_max) + later[1] * jnp.exp(
        later[0] - joined_max
    )
    return (joined_max, joined_total, earlier[2] + later[2])


def on_device(
    nx, nz, hidden, down_weight, residual, post_gain, final_gain, vocab_matrix, vocab_bias, targets
):
    rows, width = residual.shape
    count = lax.axis_size("vp")
    dp_size = lax.axis_size("dp")
    planes = dp_size // 2
    splits = 2 if rows % 32 == 0 else 1
    vp, dp = lax.axis_index("vp"), lax.axis_index("dp")
    core, plane = dp % 2, dp // 2
    units = hidden.reshape(rows, count, hidden.shape[1] // count).transpose(1, 0, 2)
    lanes = -(-rows // 128) * 128
    padded = jnp.pad(targets, (0, lanes - rows)).reshape(1, lanes)
    normed, stream, all_targets = front(
        nx, nz, splits, units, down_weight, residual,
        post_gain.reshape(1, -1), final_gain.reshape(1, -1), padded,
    )
    stream = stream.reshape(rows, width)
    tokens = 2 * count * rows
    token_rows = normed.reshape(tokens, width)
    group_targets = all_targets[:, :, 0, :rows].reshape(tokens)

    cols = vocab_matrix.shape[1] // 2
    vocab_half = lax.dynamic_slice_in_dim(vocab_matrix, core * cols, cols, 1)
    bias_half = lax.dynamic_slice_in_dim(vocab_bias, core * cols, cols, 0)
    column_ids = vp * 2 * cols + core * cols + lax.broadcasted_iota(jnp.int32, (1, cols), 1)
    hit = column_ids == group_targets[:, None]
    logits = (
        jnp.dot(token_rows, vocab_half, preferred_element_type=f32) + bias_half[None, :]
    )
    local_max = jnp.max(logits, axis=1)
    exps = jnp.exp(logits - local_max[:, None])
    stats = (local_max, jnp.sum(exps, axis=1), jnp.sum(jnp.where(hit, logits, 0.0), axis=1))
    exps = exps.astype(bf16)

    def swap(value, axis, pairs):
        return lax.ppermute(value, axis, pairs)

    core_pairs = [(d, d ^ 1) for d in range(dp_size)]
    came = swap(jnp.stack(stats), "dp", core_pairs)
    half = tokens // 2
    came = jnp.concatenate([came[:, half:], came[:, :half]], axis=1)
    stats = combine(stats, tuple(came))
    step = 1
    while step < count:
        came = swap(jnp.stack(stats), "vp", [(d, d ^ step) for d in range(count)])
        stats = combine(stats, tuple(came))
        step *= 2
    row_max, row_total, picked = stats
    log_total = row_max + jnp.log(row_total)
    factor = jnp.exp(local_max - log_total) * (1.0 + 2.0 * zloss_weight * log_total)
    dlogits = (
        exps.astype(f32) * factor[:, None] - jnp.where(hit, 1.0, 0.0)
    ).astype(bf16)
    dlogits = lax.optimization_barrier(dlogits)

    piece = width // planes
    block = piece // 2
    chunks = 4 if cols % 512 == 0 else 1
    chunk_cols = cols // chunks
    own_rows = lax.dynamic_slice_in_dim(token_rows, plane * piece, piece, 1)
    arrivals = []
    for k in range(chunks):
        column_part = dlogits[:, k * chunk_cols : (k + 1) * chunk_cols]
        got = []
        for shift in range(1, planes):
            there = (plane + shift) % planes
            grads = lax.dot_general(
                lax.dynamic_slice_in_dim(token_rows, there * piece, piece, 1), column_part,
                (((0,), (0,)), ((), ())), preferred_element_type=f32,
            ).astype(bf16)
            for c in range(2):
                part = lax.dynamic_slice_in_dim(grads, ((core + c) % 2) * block, block, 0)
                to = [
                    (d, ((d // 2 + shift) % planes) * 2 + (d % 2 + c) % 2) for d in range(dp_size)
                ]
                got.append(swap(part, "dp", to))
        arrivals.append(got)
    own = lax.dot_general(
        own_rows, dlogits, (((0,), (0,)), ((), ())), preferred_element_type=f32
    )
    kept = lax.dynamic_slice_in_dim(own, core * block, block, 0)
    given = lax.dynamic_slice_in_dim(own, (1 - core) * block, block, 0).astype(bf16)
    given = swap(given, "dp", core_pairs)
    partial = lax.dot_general(
        dlogits, vocab_half, (((1,), (1,)), ((), ())), preferred_element_type=f32
    ).astype(bf16)
    dnormed = back(nx, nz, splits, partial.reshape(normed.shape)).reshape(rows, width)

    def total(c, base):
        parts = [
            sum(arrivals[k][2 * j + c].astype(f32) for j in range(planes - 1))
            for k in range(chunks)
        ]
        return base.astype(f32) + jnp.concatenate(parts, axis=1)

    same, cross = total(0, kept), total(1, given)
    vocab_grad = jnp.concatenate(
        [jnp.where(core == 0, same, cross), jnp.where(core == 0, cross, same)], axis=1
    )
    stream_f = stream.astype(f32)
    inverse = lax.rsqrt(jnp.mean(stream_f * stream_f, axis=-1, keepdims=True) + norm_eps)
    scaled = stream_f * inverse
    all_losses = log_total - picked + zloss_weight * log_total * log_total
    losses = lax.dynamic_slice_in_dim(all_losses, vp * rows, rows, 0)
    dscaled = dnormed * final_gain[None, :]
    norm_grad = inverse * (dscaled - scaled * jnp.mean(dscaled * scaled, axis=-1, keepdims=True))
    return (losses, norm_grad, vocab_grad)


def solution(mesh):
    count = mesh.shape["vp"]
    nx = math.isqrt(count // 2)
    nx = nx if nx > 1 and count % nx == 0 else 2
    placed = (
        P(("vp", "dp"), None), P("vp", None), P(("vp", "dp"), None), P(), P(),
        P(None, "vp"), P("vp"), P(("vp", "dp")),
    )
    return jax.shard_map(
        functools.partial(on_device, nx, count // nx),
        mesh=mesh,
        in_specs=placed,
        out_specs=(P(("vp", "dp")), P(("vp", "dp"), None), P("dp", "vp")),
        check_vma=False,
    )
```

```python
import functools
import math

import jax
import jax.numpy as jnp
from jax import lax
from jax.experimental import pallas as pl
from jax.experimental.pallas import tpu as pltpu
from jax.sharding import PartitionSpec as P


norm_eps = 1e-06
zloss_weight = 0.0001
MESH = pl.DeviceIdType.MESH
f32, bf16 = jnp.float32, jnp.bfloat16


class Place:
    def __init__(self, nx, nz):
        self.nx, self.nz, self.count = nx, nz, nx * nz
        self.vp, self.dp = lax.axis_index("vp"), lax.axis_index("dp")
        self.x, self.z = lax.rem(self.vp, nx), self.vp // nx
        self.other_core = self.dp + 1 - 2 * lax.rem(self.dp, 2)

    def side(self, step):
        return lax.rem(self.x + step, self.nx)

    def at(self, x, z):
        return (z * self.nx + x, self.dp)

    def outward(self, k):
        return jnp.where(lax.rem(k, 2) == 0, k // 2, self.nz - 1 - k // 2)

    def nearby(self, k):
        low, high = self.z, self.nz - 1 - self.z
        both = jnp.minimum(low, high)
        half = (k + 1) // 2
        near = jnp.where(lax.rem(k, 2) == 1, self.z - half, self.z + half)
        far = jnp.where(high > low, self.z + (k - both), self.z - (k - both))
        return jnp.where(k <= 2 * both, near, far)


def arrived(ref, sem):
    pltpu.make_async_copy(ref, ref, sem).wait()


def send(src, dst, send_sem, recv_sem, device):
    pltpu.make_async_remote_copy(
        src_ref=src, dst_ref=dst, send_sem=send_sem, recv_sem=recv_sem,
        device_id=device, device_id_type=MESH,
    ).start()


def greet(place, everyone):
    barrier = pltpu.get_barrier_semaphore()
    for step in range(1, place.count):
        peer = lax.rem(place.vp + step, place.count)
        pl.semaphore_signal(barrier, inc=1, device_id=(peer, place.dp), device_id_type=MESH)
        if everyone:
            pl.semaphore_signal(
                barrier, inc=1, device_id=(peer, place.other_core), device_id_type=MESH
            )
    pl.semaphore_signal(
        barrier, inc=1, device_id=(place.vp, place.other_core), device_id_type=MESH
    )
    pl.semaphore_wait(barrier, place.count + (place.count - 1 if everyone else 0))


def row_loop(rows, size, body):
    @pl.loop(0, rows // size)
    def _(r):
        body(pl.ds(pl.multiple_of(r * size, size), size))


def line_reduce_scatter(place, splits, produce, px, xr, q, sb, zd, zu, sems):
    nx, nz, z = place.nx, place.nz, place.z
    xs_sem, xr_sem, zs_sem, zd_sem, zu_sem = sems
    rows = q.shape[2]
    size = min(rows, 32)

    def add(zb, s, ref):
        def body(r):
            q[zb, s, r] += ref[r].astype(f32)

        row_loop(rows, size, body)

    def pass_on(zb, s):
        def body(r):
            sb[zb, s, r] = q[zb, s, r].astype(bf16)

        row_loop(rows, size, body)

    def below(zb, s):
        @pl.when(z < nz - 1)
        def _():
            arrived(zd.at[zb, s], zd_sem.at[zb, s])
            add(zb, s, zd.at[zb, s])

    def above(zb, s):
        @pl.when(z > 0)
        def _():
            arrived(zu.at[zb, s], zu_sem.at[zb, s])
            add(zb, s, zu.at[zb, s])

    def sides(zb, s):
        for step in range(1, nx):
            arrived(xr.at[step - 1, zb, s], xr_sem.at[step - 1, zb, s])
            add(zb, s, xr.at[step - 1, zb, s])

    @pl.loop(0, nz + 1)
    def _(k):
        @pl.when(k < nz)
        def _():
            zb = place.outward(k)
            produce(zb)
            for s in range(splits):
                for step in range(1, nx):
                    slot = nx - step - 1
                    send(px.at[step - 1, zb, s], xr.at[slot, zb, s], xs_sem.at[step - 1, zb, s],
                         xr_sem.at[slot, zb, s], place.at(place.side(step), z))

        zc = place.outward(jnp.maximum(k - 1, 0))

        @pl.when((k > 0) & (zc < z))
        def _():
            for s in range(splits):
                sides(zc, s)
                below(zc, s)
                pass_on(zc, s)
                send(sb.at[zc, s], zd.at[zc, s], zs_sem.at[zc, s], zd_sem.at[zc, s],
                     place.at(place.x, z - 1))

        @pl.when((k > 0) & (zc > z))
        def _():
            for s in range(splits):
                sides(zc, s)
                above(zc, s)
                pass_on(zc, s)
                send(sb.at[zc, s], zu.at[zc, s], zs_sem.at[zc, s], zu_sem.at[zc, s],
                     place.at(place.x, z + 1))

    for s in range(splits):
        sides(z, s)
        below(z, s)
        above(z, s)

    @pl.loop(0, nz)
    def _(zb):
        for s in range(splits):
            for step in range(1, nx):
                arrived(px.at[step - 1, zb, s], xs_sem.at[step - 1, zb, s])

            @pl.when(zb != z)
            def _():
                arrived(sb.at[zb, s], zs_sem.at[zb, s])


def front_kernel(
    nx, nz, splits,
    hid, weight_in, residual, post_gain, final_gain, targets, vocab, bias,
    normed_out, dlogits_out, stream_out, losses_out,
    units, weight, px, xr, q, sb, zd, zu, normed,
    targets_out, vocab_part, scores, exps, stats, stats_in, total_own, total_in,
    xs_sem, xr_sem, zs_sem, zd_sem, zu_sem,
    hid_send, hid_recv, tgt_send, tgt_recv,
    side_send, line_send, gather_recv, core_send, core_recv, out_sem,
    weight_sem, vocab_sem, stats_send, stats_recv, total_send, total_recv, grad_sem,
):
    place = Place(nx, nz)
    count, vp, z = place.count, place.vp, place.z
    split_rows, width = q.shape[2], q.shape[3]
    rows, lanes = splits * split_rows, targets.shape[1]
    cols = vocab_part.shape[1]
    core = lax.rem(place.dp, 2)
    tile = min(cols, 512)
    vocab_load = pltpu.make_async_copy(
        vocab.at[:, pl.ds(pl.multiple_of(core * cols, cols), cols)], vocab_part, vocab_sem
    )
    weight_load = pltpu.make_async_copy(weight_in, weight, weight_sem)
    weight_load.start()
    greet(place, True)

    own = pltpu.make_async_copy(hid.at[vp], units.at[vp], hid_recv.at[vp])
    own.start()
    for k in range(count - 1):
        peer = lax.rem(vp + k + 1, count)
        send(hid.at[peer], units.at[vp], hid_send.at[k], hid_recv.at[vp], (peer, place.dp))
    for k in range(count - 1):
        peer = lax.rem(vp + k + 1, count)
        for c in range(2):
            send(targets, targets_out.at[c, vp], tgt_send.at[c, k], tgt_recv.at[c, vp],
                 (peer, place.other_core if c else place.dp))
    send(targets, targets_out.at[1, vp], tgt_send.at[1, count - 1], tgt_recv.at[1, vp],
         (vp, place.other_core))
    own_targets = pltpu.make_async_copy(targets, targets_out.at[0, vp], tgt_recv.at[0, vp])
    own_targets.start()
    vocab_load.start()
    weight_load.wait()

    def product(device, store):
        arrived(units.at[device], hid_recv.at[device])
        tile = min(width, 512)

        @pl.loop(0, width // tile)
        def _(n):
            cols = pl.ds(pl.multiple_of(n * tile, tile), tile)
            store(cols, jnp.dot(units[device], weight[:, cols], preferred_element_type=f32))

    def produce(zb):
        for step in range(nx):
            def store(cols, value):
                for s in range(splits):
                    part = value[s * split_rows : (s + 1) * split_rows]
                    if step == 0:
                        q[zb, s, :, cols] = part
                    else:
                        px[step - 1, zb, s, :, cols] = part.astype(bf16)

            product(zb * nx + place.side(step), store)

    line_reduce_scatter(
        place, splits, produce, px, xr, q, sb, zd, zu, (xs_sem, xr_sem, zs_sem, zd_sem, zu_sem)
    )

    for s in range(splits):
        def norms(r):
            mixed = q[z, s, r]
            post = mixed * lax.rsqrt(jnp.mean(mixed * mixed, axis=-1, keepdims=True) + norm_eps)
            stream = (residual[s, r].astype(f32) + post * post_gain[...]).astype(bf16)
            stream_out[s, r] = stream
            stream = stream.astype(f32)
            inverse = lax.rsqrt(jnp.mean(stream * stream, axis=-1, keepdims=True) + norm_eps)
            normed[0, vp, s, r] = (stream * inverse * final_gain[...]).astype(bf16)

        row_loop(split_rows, 16, norms)

    blocks, block_width = normed_out.shape[0], normed_out.shape[-1]
    plane = place.dp // 2

    def keep(c, i, s):
        for b in range(blocks):
            there = lax.rem(plane + b // 2, blocks // 2)
            at = (there * 2 + lax.rem(core + b, 2)) * block_width
            pltpu.make_async_copy(
                normed.at[c, i, s, :, pl.ds(pl.multiple_of(at, block_width), block_width)],
                normed_out.at[b, c, i, s], out_sem.at[c, i, s],
            ).start()

    def to_core(i, s):
        keep(0, i, s)
        send(normed.at[0, i, s], normed.at[1, i, s], core_send.at[i, s], core_recv.at[i, s],
             (vp, place.other_core))

    @pl.loop(0, count)
    def _(i):
        for c in range(2):
            arrived(targets_out.at[c, i], tgt_recv.at[c, i])

    vocab_load.wait()
    first_column = vp * 2 * cols + core * cols

    def column_of(row):
        return jnp.transpose(jnp.broadcast_to(row, (128, lanes)))[:rows, :1]

    def row_of(column):
        return jnp.transpose(jnp.broadcast_to(column, (rows, 128)))[:1, :]

    def score(i):
        for s in range(splits):
            arrived(normed.at[1, i, s], core_recv.at[i, s])
            keep(1, i, s)
        block = jnp.concatenate(
            [normed[c, i, s] for c in range(2) for s in range(splits)], axis=0
        )
        high = jnp.full((2 * rows, 1), -jnp.inf, f32)
        for n in range(cols // tile):
            at = slice(n * tile, (n + 1) * tile)
            value = jnp.dot(block, vocab_part[:, at], preferred_element_type=f32) + bias[:, at]
            scores[:, at] = value
            high = jnp.maximum(high, jnp.max(value, axis=1, keepdims=True))
        for c in range(2):
            part = slice(c * rows, (c + 1) * rows)
            target = column_of(targets_out[c, i]) - first_column
            top = high[part]
            total = jnp.zeros((rows, 1), f32)
            picked = jnp.zeros((rows, 1), f32)
            for n in range(cols // tile):
                at = slice(n * tile, (n + 1) * tile)
                value = scores[part, at]
                ids = n * tile + lax.broadcasted_iota(jnp.int32, (rows, tile), 1)
                raised = jnp.exp(value - top)
                total += jnp.sum(raised, axis=1, keepdims=True)
                picked += jnp.sum(jnp.where(ids == target, value, 0.0), axis=1, keepdims=True)
                exps[c, i, :, at] = raised.astype(bf16)
            for j, value in enumerate((top, total, picked)):
                stats[c, i, j : j + 1, :rows] = row_of(value)

        @pl.when(i != vp)
        def _():
            for c in range(2):
                send(stats.at[c, i], stats_in.at[c, vp], stats_send.at[c, i], stats_recv.at[c, vp],
                     (i, place.other_core if c else place.dp))

        @pl.when(i == vp)
        def _():
            send(stats.at[1, i], stats_in.at[1, vp], stats_send.at[1, i], stats_recv.at[1, vp],
                 (vp, place.other_core))
            pltpu.make_async_copy(stats.at[0, i], stats_in.at[0, vp], stats_recv.at[0, vp]).start()

    @pl.loop(0, nz + 1)
    def _(k):
        @pl.when(k < nz)
        def _():
            zb = place.nearby(k)
            i = zb * nx + place.x
            for s in range(splits):
                block, sem = normed.at[0, i, s], gather_recv.at[i, s]

                @pl.when(k > 0)
                def _():
                    arrived(block, sem)

                @pl.when((zb >= z) & (z > 0))
                def _():
                    send(block, block, line_send.at[0, zb, s], sem, place.at(place.x, z - 1))

                @pl.when((zb <= z) & (z < nz - 1))
                def _():
                    send(block, block, line_send.at[1, zb, s], sem, place.at(place.x, z + 1))

                for step in range(1, nx):
                    send(block, block, side_send.at[step - 1, zb, s], sem,
                         place.at(place.side(step), z))
                to_core(i, s)

        @pl.when(k > 0)
        def _():
            zb = place.nearby(k - 1)
            for step in range(1, nx):
                i = zb * nx + place.side(step)
                for s in range(splits):
                    arrived(normed.at[0, i, s], gather_recv.at[i, s])
                    to_core(i, s)

        @pl.loop(0, nx)
        def _(step):
            @pl.when(((step == 0) & (k < nz)) | ((step > 0) & (k > 0)))
            def _():
                zb = place.nearby(jnp.where(step == 0, jnp.minimum(k, nz - 1), jnp.maximum(k - 1, 0)))
                score(zb * nx + place.side(step))

    @pl.loop(0, count)
    def _(i):
        for c in range(2):
            arrived(stats_in.at[c, i], stats_recv.at[c, i])

    pairs = [(c, i) for c in range(2) for i in range(count)]
    top = stats_in[0, 0, 0:1]
    for c, i in pairs[1:]:
        top = jnp.maximum(top, stats_in[c, i, 0:1])
    total = jnp.zeros((1, lanes), f32)
    picked = jnp.zeros((1, lanes), f32)
    for c, i in pairs:
        total += stats_in[c, i, 1:2] * jnp.exp(stats_in[c, i, 0:1] - top)
        picked += stats_in[c, i, 2:3]
    log_total = top + jnp.log(total)
    total_own[...] = log_total
    losses_out[...] = log_total - picked + zloss_weight * log_total * log_total
    for k in range(count - 1):
        peer = lax.rem(vp + k + 1, count)
        for c in range(2):
            send(total_own, total_in.at[c, vp], total_send.at[c, k], total_recv.at[c, vp],
                 (peer, place.other_core if c else place.dp))
    send(total_own, total_in.at[1, vp], total_send.at[1, count - 1], total_recv.at[1, vp],
         (vp, place.other_core))
    pltpu.make_async_copy(total_own, total_in.at[0, vp], total_recv.at[0, vp]).start()

    @pl.loop(0, count)
    def _(k):
        i = lax.rem(vp + k, count)
        for c in range(2):
            arrived(total_in.at[c, i], total_recv.at[c, i])
            log_total = total_in[c, i]
            factor = jnp.exp(stats[c, i, 0:1] - log_total) * (1.0 + 2.0 * zloss_weight * log_total)
            factor = column_of(factor)
            target = column_of(targets_out[c, i]) - first_column
            for n in range(cols // tile):
                at = slice(n * tile, (n + 1) * tile)
                ids = n * tile + lax.broadcasted_iota(jnp.int32, (rows, tile), 1)
                value = exps[c, i, :, at].astype(f32) * factor - jnp.where(ids == target, 1.0, 0.0)
                exps[c, i, :, at] = value.astype(bf16)
            pltpu.make_async_copy(exps.at[c, i], dlogits_out.at[c, i], grad_sem.at[c, i]).start()

    @pl.loop(0, nz)
    def _(zb):
        for s in range(splits):
            block = normed.at[0, zb * nx + place.x, s]

            @pl.when((zb >= z) & (z > 0))
            def _():
                arrived(block, line_send.at[0, zb, s])

            @pl.when((zb <= z) & (z < nz - 1))
            def _():
                arrived(block, line_send.at[1, zb, s])

            for step in range(1, nx):
                arrived(block, side_send.at[step - 1, zb, s])

    @pl.loop(0, count)
    def _(i):
        for s in range(splits):
            arrived(normed.at[0, i, s], core_send.at[i, s])
            for c in range(2):
                arrived(normed.at[c, i, s], out_sem.at[c, i, s])

    @pl.loop(0, count)
    def _(i):
        for c in range(2):
            arrived(exps.at[c, i], grad_sem.at[c, i])
        arrived(stats.at[1, i], stats_send.at[1, i])

        @pl.when(i != vp)
        def _():
            arrived(stats.at[0, i], stats_send.at[0, i])

    for k in range(count - 1):
        arrived(hid.at[0], hid_send.at[k])
        for c in range(2):
            arrived(targets, tgt_send.at[c, k])
            arrived(total_own, total_send.at[c, k])
    arrived(targets, tgt_send.at[1, count - 1])
    arrived(total_own, total_send.at[1, count - 1])


def rs_scratch(nx, nz, splits, rows, width):
    shape = (nz, splits, rows, width)
    return [
        pltpu.VMEM((nx - 1,) + shape, bf16),
        pltpu.VMEM((nx - 1,) + shape, bf16),
        pltpu.VMEM(shape, f32),
        pltpu.VMEM(shape, bf16),
        pltpu.VMEM(shape, bf16),
        pltpu.VMEM(shape, bf16),
    ]


def rs_sems(nx, nz, splits):
    dma = pltpu.SemaphoreType.DMA
    return [dma((nx - 1, nz, splits))] * 2 + [dma((nz, splits))] * 3


def front(nx, nz, splits, blocks, hid, weight, residual, post_gain, final_gain, targets, vocab, bias):
    count, rows, _ = hid.shape
    width = weight.shape[1]
    split_rows = rows // splits
    dma = pltpu.SemaphoreType.DMA
    vmem = pl.BlockSpec(memory_space=pltpu.VMEM)
    hbm = pl.BlockSpec(memory_space=pl.ANY)
    cols, lanes = bias.shape[1], targets.shape[1]
    flops = 2 * count * rows * weight.shape[0] * width
    return pl.pallas_call(
        functools.partial(front_kernel, nx, nz, splits),
        out_shape=(
            jax.ShapeDtypeStruct((blocks, 2, count, splits, split_rows, width // blocks), bf16),
            jax.ShapeDtypeStruct((2, count, rows, cols), bf16),
            jax.ShapeDtypeStruct((splits, split_rows, width), bf16),
            jax.ShapeDtypeStruct((1, lanes), f32),
        ),
        in_specs=[hbm] * 2 + [vmem] * 4 + [hbm, vmem],
        out_specs=(hbm, hbm, vmem, vmem),
        scratch_shapes=[pltpu.VMEM(hid.shape, bf16), pltpu.VMEM(weight.shape, bf16)]
        + rs_scratch(nx, nz, splits, split_rows, width)
        + [
            pltpu.VMEM((2, count, splits, split_rows, width), bf16),
            pltpu.VMEM((2, count, 1, lanes), jnp.int32),
            pltpu.VMEM((width, cols), bf16),
            pltpu.VMEM((2 * rows, cols), f32),
            pltpu.VMEM((2, count, rows, cols), bf16),
            pltpu.VMEM((2, count, 8, lanes), f32),
            pltpu.VMEM((2, count, 8, lanes), f32),
            pltpu.VMEM((1, lanes), f32),
            pltpu.VMEM((2, count, 1, lanes), f32),
        ]
        + rs_sems(nx, nz, splits)
        + [
            dma((count - 1,)), dma((count,)), dma((2, count)), dma((2, count)),
            dma((nx - 1, nz, splits)), dma((2, nz, splits)), dma((count, splits)),
            dma((count, splits)), dma((count, splits)), dma((2, count, splits)),
            dma, dma, dma((2, count)), dma((2, count)), dma((2, count)), dma((2, count)),
            dma((2, count)),
        ],
        compiler_params=pltpu.CompilerParams(
            collective_id=0, has_side_effects=True, vmem_limit_bytes=60 << 20
        ),
        cost_estimate=pl.CostEstimate(flops=flops, bytes_accessed=1 << 24, transcendentals=0),
        name="front",
    )(hid, weight, residual.reshape(splits, split_rows, width), post_gain, final_gain, targets,
      vocab, bias)


def back_kernel(
    nx, nz, splits,
    dlogits, vocab, own_out,
    grads, vocab_part, terms, given, theirs, px, xr, q, sb, zd, zu,
    xs_sem, xr_sem, zs_sem, zd_sem, zu_sem,
    load_sem, vocab_sem, core_send, core_recv,
):
    place = Place(nx, nz)
    count, z = place.count, place.z
    split_rows = q.shape[2]
    rows = splits * split_rows
    cols = vocab_part.shape[2]
    pieces, piece = vocab_part.shape[0], vocab_part.shape[1]
    core = lax.rem(place.dp, 2)
    greet(place, False)

    def load(zb):
        for step in range(nx):
            i = zb * nx + place.side(step)
            for c in range(2):
                pltpu.make_async_copy(dlogits.at[c, i], grads.at[c, i], load_sem.at[c, i]).start()

    load(0)
    for n in range(pieces):
        pltpu.make_async_copy(
            vocab.at[n * piece : (n + 1) * piece, pl.ds(pl.multiple_of(core * cols, cols), cols)],
            vocab_part.at[n], vocab_sem.at[n],
        ).start()

    @pl.loop(1, nz)
    def _(k):
        load(place.outward(k))

    def produce(zb):
        for step in range(nx):
            i = zb * nx + place.side(step)
            for c in range(2):
                arrived(grads.at[c, i], load_sem.at[c, i])
            block = jnp.concatenate([grads[0, i], grads[1, i]], axis=0)

            @pl.loop(0, pieces)
            def _(n):
                if step == 0:
                    @pl.when(zb == 0)
                    def _():
                        arrived(vocab_part.at[n], vocab_sem.at[n])

                at = pl.ds(pl.multiple_of(n * piece, piece), piece)
                value = lax.dot_general(
                    block, vocab_part[n], (((1,), (1,)), ((), ())), preferred_element_type=f32
                )
                for s in range(splits):
                    r = s * split_rows
                    terms[step, s, :, at] = value[r : r + split_rows]
                    given[i, s, :, at] = value[rows + r : rows + r + split_rows].astype(bf16)

            for s in range(splits):
                send(given.at[i, s], theirs.at[i, s], core_send.at[i, s], core_recv.at[i, s],
                     (place.vp, place.other_core))
        for step in range(nx):
            i = zb * nx + place.side(step)
            for s in range(splits):
                arrived(theirs.at[i, s], core_recv.at[i, s])

                def body(r):
                    value = terms[step, s, r] + theirs[i, s, r].astype(f32)
                    if step == 0:
                        q[zb, s, r] = value
                    else:
                        px[step - 1, zb, s, r] = value.astype(bf16)

                row_loop(split_rows, 16, body)

    line_reduce_scatter(
        place, splits, produce, px, xr, q, sb, zd, zu, (xs_sem, xr_sem, zs_sem, zd_sem, zu_sem)
    )
    for s in range(splits):
        def body(r):
            own_out[s, r] = q[z, s, r]

        row_loop(split_rows, 16, body)

    @pl.loop(0, count)
    def _(i):
        for s in range(splits):
            arrived(given.at[i, s], core_send.at[i, s])


def back(nx, nz, splits, dlogits, vocab):
    _, count, rows, cols = dlogits.shape
    width = vocab.shape[0]
    split_rows = rows // splits
    piece = math.gcd(width, 512)
    dma = pltpu.SemaphoreType.DMA
    shape = (count, splits, split_rows, width)
    hbm = pl.BlockSpec(memory_space=pl.ANY)
    return pl.pallas_call(
        functools.partial(back_kernel, nx, nz, splits),
        out_shape=jax.ShapeDtypeStruct((splits, split_rows, width), f32),
        in_specs=[hbm, hbm],
        out_specs=pl.BlockSpec(memory_space=pltpu.VMEM),
        scratch_shapes=[
            pltpu.VMEM((2, count, rows, cols), bf16),
            pltpu.VMEM((width // piece, piece, cols), bf16),
            pltpu.VMEM((nx, splits, split_rows, width), f32),
            pltpu.VMEM(shape, bf16),
            pltpu.VMEM(shape, bf16),
        ]
        + rs_scratch(nx, nz, splits, split_rows, width)
        + rs_sems(nx, nz, splits)
        + [dma((2, count)), dma((width // piece,)), dma((count, splits)), dma((count, splits))],
        compiler_params=pltpu.CompilerParams(
            collective_id=1, has_side_effects=True, vmem_limit_bytes=56 << 20
        ),
        cost_estimate=pl.CostEstimate(
            flops=4 * count * rows * cols * width, bytes_accessed=1 << 24, transcendentals=0
        ),
        name="back",
    )(dlogits, vocab)


def on_device(
    nx, nz, hidden, down_weight, residual, post_gain, final_gain, vocab_matrix, vocab_bias, targets
):
    rows, width = residual.shape
    count = lax.axis_size("vp")
    dp_size = lax.axis_size("dp")
    planes = dp_size // 2
    splits = 4 if rows % 64 == 0 else 2 if rows % 32 == 0 else 1
    core = lax.axis_index("dp") % 2
    units = hidden.reshape(rows, count, hidden.shape[1] // count).transpose(1, 0, 2)
    lanes = -(-rows // 128) * 128
    padded = jnp.pad(targets, (0, lanes - rows)).reshape(1, lanes)
    cols = vocab_matrix.shape[1] // 2
    bias_half = lax.dynamic_slice_in_dim(vocab_bias, core * cols, cols, 0)
    normed, dlogits, stream, losses = front(
        nx, nz, splits, 2 * planes, units, down_weight, residual,
        post_gain.reshape(1, -1), final_gain.reshape(1, -1), padded,
        vocab_matrix, bias_half.reshape(1, -1),
    )
    stream = stream.reshape(rows, width)
    tokens = 2 * count * rows
    token_rows = normed.reshape(2 * planes, tokens, width // (2 * planes))
    dlogits_2d = dlogits.reshape(tokens, cols)

    core_pairs = [(d, d ^ 1) for d in range(dp_size)]
    spans = column_spans(cols)
    arrivals = []
    source = dlogits_2d
    for low, high in spans:
        got = []
        for shift in range(1, planes):
            for c in range(2):
                grads = lax.dot_general(
                    token_rows[2 * shift + c], source[:, low:high],
                    (((0,), (0,)), ((), ())), preferred_element_type=f32,
                ).astype(bf16)
                grads, source = lax.optimization_barrier((grads, source))
                to = [
                    (d, ((d // 2 + shift) % planes) * 2 + (d % 2 + c) % 2) for d in range(dp_size)
                ]
                got.append(lax.ppermute(grads, "dp", to))
        arrivals.append(got)
    dnormed = back(nx, nz, splits, source.reshape(dlogits.shape), vocab_matrix)
    dnormed, source = lax.optimization_barrier((dnormed, source))
    dnormed = dnormed.reshape(rows, width)
    halves = [
        lax.dot_general(
            token_rows[c], source, (((0,), (0,)), ((), ())), preferred_element_type=f32,
        )
        for c in (1, 0)
    ]
    given = lax.ppermute(halves[0].astype(bf16), "dp", core_pairs)
    kept = halves[1]

    def total(c, base):
        parts = [
            sum(arrivals[k][2 * j + c].astype(f32) for j in range(planes - 1))
            for k in range(len(spans))
        ]
        return base.astype(f32) + jnp.concatenate(parts, axis=1)

    same, cross = total(0, kept), total(1, given)
    vocab_grad = jnp.concatenate(
        [jnp.where(core == 0, same, cross), jnp.where(core == 0, cross, same)], axis=1
    )
    stream_f = stream.astype(f32)
    inverse = lax.rsqrt(jnp.mean(stream_f * stream_f, axis=-1, keepdims=True) + norm_eps)
    scaled = stream_f * inverse
    dscaled = dnormed * final_gain[None, :]
    norm_grad = inverse * (dscaled - scaled * jnp.mean(dscaled * scaled, axis=-1, keepdims=True))
    return (losses[0, :rows], norm_grad, vocab_grad)


def column_spans(cols):
    first = 512
    return ((0, first), (first, cols)) if cols > first else ((0, cols),)


def solution(mesh):
    count = mesh.shape["vp"]
    nx = math.isqrt(count // 2)
    nx = nx if nx > 1 and count % nx == 0 else 2
    placed = (
        P(("vp", "dp"), None), P("vp", None), P(("vp", "dp"), None), P(), P(),
        P(None, "vp"), P("vp"), P(("vp", "dp")),
    )
    return jax.shard_map(
        functools.partial(on_device, nx, count // nx),
        mesh=mesh,
        in_specs=placed,
        out_specs=(P(("vp", "dp")), P(("vp", "dp"), None), P("dp", "vp")),
        check_vma=False,
    )
```

```python
import functools
import math

import jax
import jax.numpy as jnp
from jax import lax
from jax.experimental import pallas as pl
from jax.experimental.pallas import tpu as pltpu
from jax.sharding import PartitionSpec as P


norm_eps = 1e-06
zloss_weight = 0.0001
MESH = pl.DeviceIdType.MESH
f32, bf16 = jnp.float32, jnp.bfloat16


class Place:
    def __init__(self, nx, nz):
        self.nx, self.nz, self.count = nx, nz, nx * nz
        self.vp, self.dp = lax.axis_index("vp"), lax.axis_index("dp")
        self.x, self.z = lax.rem(self.vp, nx), self.vp // nx
        self.other_core = self.dp + 1 - 2 * lax.rem(self.dp, 2)

    def side(self, step):
        return lax.rem(self.x + step, self.nx)

    def at(self, x, z):
        return (z * self.nx + x, self.dp)

    def outward(self, k):
        return jnp.where(lax.rem(k, 2) == 0, k // 2, self.nz - 1 - k // 2)

    def nearby(self, k):
        low, high = self.z, self.nz - 1 - self.z
        both = jnp.minimum(low, high)
        half = (k + 1) // 2
        near = jnp.where(lax.rem(k, 2) == 1, self.z - half, self.z + half)
        far = jnp.where(high > low, self.z + (k - both), self.z - (k - both))
        return jnp.where(k <= 2 * both, near, far)


def arrived(ref, sem):
    pltpu.make_async_copy(ref, ref, sem).wait()


def send(src, dst, send_sem, recv_sem, device):
    pltpu.make_async_remote_copy(
        src_ref=src, dst_ref=dst, send_sem=send_sem, recv_sem=recv_sem,
        device_id=device, device_id_type=MESH,
    ).start()


def greet(place, everyone):
    barrier = pltpu.get_barrier_semaphore()
    for step in range(1, place.count):
        peer = lax.rem(place.vp + step, place.count)
        pl.semaphore_signal(barrier, inc=1, device_id=(peer, place.dp), device_id_type=MESH)
        if everyone:
            pl.semaphore_signal(
                barrier, inc=1, device_id=(peer, place.other_core), device_id_type=MESH
            )
    pl.semaphore_signal(
        barrier, inc=1, device_id=(place.vp, place.other_core), device_id_type=MESH
    )
    pl.semaphore_wait(barrier, place.count + (place.count - 1 if everyone else 0))


def row_loop(rows, size, body):
    @pl.loop(0, rows // size)
    def _(r):
        body(pl.ds(pl.multiple_of(r * size, size), size))


def line_reduce_scatter(place, splits, produce, px, xr, q, sb, zd, zu, sems, meanwhile=None):
    nx, nz, z = place.nx, place.nz, place.z
    xs_sem, xr_sem, zs_sem, zd_sem, zu_sem = sems
    rows = q.shape[2]
    size = min(rows, 32)

    def add(zb, s, ref):
        def body(r):
            q[zb, s, r] += ref[r].astype(f32)

        row_loop(rows, size, body)

    def pass_on(zb, s):
        def body(r):
            sb[zb, s, r] = q[zb, s, r].astype(bf16)

        row_loop(rows, size, body)

    def below(zb, s):
        @pl.when(z < nz - 1)
        def _():
            arrived(zd.at[zb, s], zd_sem.at[zb, s])
            add(zb, s, zd.at[zb, s])

    def above(zb, s):
        @pl.when(z > 0)
        def _():
            arrived(zu.at[zb, s], zu_sem.at[zb, s])
            add(zb, s, zu.at[zb, s])

    def sides(zb, s):
        for step in range(1, nx):
            arrived(xr.at[step - 1, zb, s], xr_sem.at[step - 1, zb, s])
            add(zb, s, xr.at[step - 1, zb, s])

    @pl.loop(0, nz + 1)
    def _(k):
        @pl.when(k < nz)
        def _():
            zb = place.outward(k)
            produce(zb)
            for s in range(splits):
                for step in range(1, nx):
                    slot = nx - step - 1
                    send(px.at[step - 1, zb, s], xr.at[slot, zb, s], xs_sem.at[step - 1, zb, s],
                         xr_sem.at[slot, zb, s], place.at(place.side(step), z))

        if meanwhile is not None:
            meanwhile(k)

        zc = place.outward(jnp.maximum(k - 1, 0))

        @pl.when((k > 0) & (zc < z))
        def _():
            for s in range(splits):
                sides(zc, s)
                below(zc, s)
                pass_on(zc, s)
                send(sb.at[zc, s], zd.at[zc, s], zs_sem.at[zc, s], zd_sem.at[zc, s],
                     place.at(place.x, z - 1))

        @pl.when((k > 0) & (zc > z))
        def _():
            for s in range(splits):
                sides(zc, s)
                above(zc, s)
                pass_on(zc, s)
                send(sb.at[zc, s], zu.at[zc, s], zs_sem.at[zc, s], zu_sem.at[zc, s],
                     place.at(place.x, z + 1))

    if meanwhile is not None:
        meanwhile(None)
    for s in range(splits):
        sides(z, s)
        below(z, s)
        above(z, s)

    @pl.loop(0, nz)
    def _(zb):
        for s in range(splits):
            for step in range(1, nx):
                arrived(px.at[step - 1, zb, s], xs_sem.at[step - 1, zb, s])

            @pl.when(zb != z)
            def _():
                arrived(sb.at[zb, s], zs_sem.at[zb, s])


def front_kernel(
    nx, nz, splits, blocks,
    hid, weight_in, residual, post_gain, final_gain, targets, vocab, bias,
    *refs,
):
    normed_out, refs = refs[:blocks], refs[blocks:]
    (
        dlogits_out, stream_out, losses_out,
        units, weight, px, xr, q, sb, zd, zu, normed,
        targets_out, vocab_part, scores, exps, stats, stats_in, total_own, total_in,
        xs_sem, xr_sem, zs_sem, zd_sem, zu_sem,
        hid_send, hid_recv, tgt_send, tgt_recv,
        side_send, line_send, gather_recv, core_send, core_recv, out_sem,
        weight_sem, vocab_sem, stats_send, stats_recv, total_send, total_recv, grad_sem,
    ) = refs
    place = Place(nx, nz)
    count, vp, z = place.count, place.vp, place.z
    split_rows, width = q.shape[2], q.shape[3]
    rows, lanes = splits * split_rows, targets.shape[1]
    cols = vocab_part.shape[1]
    core = lax.rem(place.dp, 2)
    tile = min(cols, 512)
    vocab_load = pltpu.make_async_copy(
        vocab.at[:, pl.ds(pl.multiple_of(core * cols, cols), cols)], vocab_part, vocab_sem
    )
    weight_load = pltpu.make_async_copy(weight_in, weight, weight_sem)
    weight_load.start()
    greet(place, True)

    own = pltpu.make_async_copy(hid.at[vp], units.at[vp], hid_recv.at[vp])
    own.start()
    for k in range(count - 1):
        peer = lax.rem(vp + k + 1, count)
        send(hid.at[peer], units.at[vp], hid_send.at[k], hid_recv.at[vp], (peer, place.dp))
    for k in range(count - 1):
        peer = lax.rem(vp + k + 1, count)
        for c in range(2):
            send(targets, targets_out.at[c, vp], tgt_send.at[c, k], tgt_recv.at[c, vp],
                 (peer, place.other_core if c else place.dp))
    send(targets, targets_out.at[1, vp], tgt_send.at[1, count - 1], tgt_recv.at[1, vp],
         (vp, place.other_core))
    own_targets = pltpu.make_async_copy(targets, targets_out.at[0, vp], tgt_recv.at[0, vp])
    own_targets.start()
    vocab_load.start()
    weight_load.wait()

    def product(device, store):
        arrived(units.at[device], hid_recv.at[device])
        tile = min(width, 512)

        @pl.loop(0, width // tile)
        def _(n):
            cols = pl.ds(pl.multiple_of(n * tile, tile), tile)
            store(cols, jnp.dot(units[device], weight[:, cols], preferred_element_type=f32))

    def produce(zb):
        for step in range(nx):
            def store(cols, value):
                for s in range(splits):
                    part = value[s * split_rows : (s + 1) * split_rows]
                    if step == 0:
                        q[zb, s, :, cols] = part
                    else:
                        px[step - 1, zb, s, :, cols] = part.astype(bf16)

            product(zb * nx + place.side(step), store)

    line_reduce_scatter(
        place, splits, produce, px, xr, q, sb, zd, zu, (xs_sem, xr_sem, zs_sem, zd_sem, zu_sem)
    )

    for s in range(splits):
        def norms(r):
            mixed = q[z, s, r]
            post = mixed * lax.rsqrt(jnp.mean(mixed * mixed, axis=-1, keepdims=True) + norm_eps)
            stream = (residual[s, r].astype(f32) + post * post_gain[...]).astype(bf16)
            stream_out[s, r] = stream
            stream = stream.astype(f32)
            inverse = lax.rsqrt(jnp.mean(stream * stream, axis=-1, keepdims=True) + norm_eps)
            normed[0, vp, s, r] = (stream * inverse * final_gain[...]).astype(bf16)

        row_loop(split_rows, 16, norms)

    block_width = width // blocks
    plane = place.dp // 2

    def keep(c, i, s):
        for b in range(blocks):
            there = lax.rem(plane + b // 2, blocks // 2)
            at = (there * 2 + lax.rem(core + b, 2)) * block_width
            pltpu.make_async_copy(
                normed.at[c, i, s, :, pl.ds(pl.multiple_of(at, block_width), block_width)],
                normed_out[b].at[c, i, s], out_sem.at[c, i, s],
            ).start()

    def to_core(i, s):
        keep(0, i, s)
        send(normed.at[0, i, s], normed.at[1, i, s], core_send.at[i, s], core_recv.at[i, s],
             (vp, place.other_core))

    @pl.loop(0, count)
    def _(i):
        for c in range(2):
            arrived(targets_out.at[c, i], tgt_recv.at[c, i])

    vocab_load.wait()
    first_column = vp * 2 * cols + core * cols

    def column_of(row):
        return jnp.transpose(jnp.broadcast_to(row, (128, lanes)))[:rows, :1]

    def row_of(column):
        return jnp.transpose(jnp.broadcast_to(column, (rows, 128)))[:1, :]

    def score(i):
        for s in range(splits):
            arrived(normed.at[1, i, s], core_recv.at[i, s])
            keep(1, i, s)
        block = jnp.concatenate(
            [normed[c, i, s] for c in range(2) for s in range(splits)], axis=0
        )
        high = jnp.full((2 * rows, 1), -jnp.inf, f32)
        for n in range(cols // tile):
            at = slice(n * tile, (n + 1) * tile)
            value = jnp.dot(block, vocab_part[:, at], preferred_element_type=f32) + bias[:, at]
            scores[:, at] = value
            high = jnp.maximum(high, jnp.max(value, axis=1, keepdims=True))
        for c in range(2):
            part = slice(c * rows, (c + 1) * rows)
            target = column_of(targets_out[c, i]) - first_column
            top = high[part]
            total = jnp.zeros((rows, 1), f32)
            picked = jnp.zeros((rows, 1), f32)
            for n in range(cols // tile):
                at = slice(n * tile, (n + 1) * tile)
                value = scores[part, at]
                ids = n * tile + lax.broadcasted_iota(jnp.int32, (rows, tile), 1)
                raised = jnp.exp(value - top)
                total += jnp.sum(raised, axis=1, keepdims=True)
                picked += jnp.sum(jnp.where(ids == target, value, 0.0), axis=1, keepdims=True)
                exps[c, i, :, at] = raised.astype(bf16)
            for j, value in enumerate((top, total, picked)):
                stats[c, i, j : j + 1, :rows] = row_of(value)

        @pl.when(i != vp)
        def _():
            for c in range(2):
                send(stats.at[c, i], stats_in.at[c, vp], stats_send.at[c, i], stats_recv.at[c, vp],
                     (i, place.other_core if c else place.dp))

        @pl.when(i == vp)
        def _():
            send(stats.at[1, i], stats_in.at[1, vp], stats_send.at[1, i], stats_recv.at[1, vp],
                 (vp, place.other_core))
            pltpu.make_async_copy(stats.at[0, i], stats_in.at[0, vp], stats_recv.at[0, vp]).start()

    @pl.loop(0, nz + 1)
    def _(k):
        @pl.when(k < nz)
        def _():
            zb = place.nearby(k)
            i = zb * nx + place.x
            for s in range(splits):
                block, sem = normed.at[0, i, s], gather_recv.at[i, s]

                @pl.when(k > 0)
                def _():
                    arrived(block, sem)

                @pl.when((zb >= z) & (z > 0))
                def _():
                    send(block, block, line_send.at[0, zb, s], sem, place.at(place.x, z - 1))

                @pl.when((zb <= z) & (z < nz - 1))
                def _():
                    send(block, block, line_send.at[1, zb, s], sem, place.at(place.x, z + 1))

                for step in range(1, nx):
                    send(block, block, side_send.at[step - 1, zb, s], sem,
                         place.at(place.side(step), z))
                to_core(i, s)

        @pl.when(k > 0)
        def _():
            zb = place.nearby(k - 1)
            for step in range(1, nx):
                i = zb * nx + place.side(step)
                for s in range(splits):
                    arrived(normed.at[0, i, s], gather_recv.at[i, s])
                    to_core(i, s)

        @pl.loop(0, nx)
        def _(step):
            @pl.when(((step == 0) & (k < nz)) | ((step > 0) & (k > 0)))
            def _():
                zb = place.nearby(jnp.where(step == 0, jnp.minimum(k, nz - 1), jnp.maximum(k - 1, 0)))
                score(zb * nx + place.side(step))

    @pl.loop(0, count)
    def _(i):
        for c in range(2):
            arrived(stats_in.at[c, i], stats_recv.at[c, i])

    pairs = [(c, i) for c in range(2) for i in range(count)]
    top = stats_in[0, 0, 0:1]
    for c, i in pairs[1:]:
        top = jnp.maximum(top, stats_in[c, i, 0:1])
    total = jnp.zeros((1, lanes), f32)
    picked = jnp.zeros((1, lanes), f32)
    for c, i in pairs:
        total += stats_in[c, i, 1:2] * jnp.exp(stats_in[c, i, 0:1] - top)
        picked += stats_in[c, i, 2:3]
    log_total = top + jnp.log(total)
    total_own[...] = log_total
    losses_out[...] = log_total - picked + zloss_weight * log_total * log_total
    for k in range(count - 1):
        peer = lax.rem(vp + k + 1, count)
        for c in range(2):
            send(total_own, total_in.at[c, vp], total_send.at[c, k], total_recv.at[c, vp],
                 (peer, place.other_core if c else place.dp))
    send(total_own, total_in.at[1, vp], total_send.at[1, count - 1], total_recv.at[1, vp],
         (vp, place.other_core))
    pltpu.make_async_copy(total_own, total_in.at[0, vp], total_recv.at[0, vp]).start()

    @pl.loop(0, count)
    def _(k):
        i = lax.rem(vp + k, count)
        for c in range(2):
            arrived(total_in.at[c, i], total_recv.at[c, i])
            log_total = total_in[c, i]
            factor = jnp.exp(stats[c, i, 0:1] - log_total) * (1.0 + 2.0 * zloss_weight * log_total)
            factor = column_of(factor)
            target = column_of(targets_out[c, i]) - first_column
            for n in range(cols // tile):
                at = slice(n * tile, (n + 1) * tile)
                ids = n * tile + lax.broadcasted_iota(jnp.int32, (rows, tile), 1)
                value = exps[c, i, :, at].astype(f32) * factor - jnp.where(ids == target, 1.0, 0.0)
                exps[c, i, :, at] = value.astype(bf16)
            pltpu.make_async_copy(exps.at[c, i], dlogits_out.at[c, i], grad_sem.at[c, i]).start()

    @pl.loop(0, nz)
    def _(zb):
        for s in range(splits):
            block = normed.at[0, zb * nx + place.x, s]

            @pl.when((zb >= z) & (z > 0))
            def _():
                arrived(block, line_send.at[0, zb, s])

            @pl.when((zb <= z) & (z < nz - 1))
            def _():
                arrived(block, line_send.at[1, zb, s])

            for step in range(1, nx):
                arrived(block, side_send.at[step - 1, zb, s])

    @pl.loop(0, count)
    def _(i):
        for s in range(splits):
            arrived(normed.at[0, i, s], core_send.at[i, s])
            for c in range(2):
                arrived(normed.at[c, i, s], out_sem.at[c, i, s])

    @pl.loop(0, count)
    def _(i):
        for c in range(2):
            arrived(exps.at[c, i], grad_sem.at[c, i])
        arrived(stats.at[1, i], stats_send.at[1, i])

        @pl.when(i != vp)
        def _():
            arrived(stats.at[0, i], stats_send.at[0, i])

    for k in range(count - 1):
        arrived(hid.at[0], hid_send.at[k])
        for c in range(2):
            arrived(targets, tgt_send.at[c, k])
            arrived(total_own, total_send.at[c, k])
    arrived(targets, tgt_send.at[1, count - 1])
    arrived(total_own, total_send.at[1, count - 1])


def rs_scratch(nx, nz, splits, rows, width):
    shape = (nz, splits, rows, width)
    return [
        pltpu.VMEM((nx - 1,) + shape, bf16),
        pltpu.VMEM((nx - 1,) + shape, bf16),
        pltpu.VMEM(shape, f32),
        pltpu.VMEM(shape, bf16),
        pltpu.VMEM(shape, bf16),
        pltpu.VMEM(shape, bf16),
    ]


def rs_sems(nx, nz, splits):
    dma = pltpu.SemaphoreType.DMA
    return [dma((nx - 1, nz, splits))] * 2 + [dma((nz, splits))] * 3


def front(nx, nz, splits, blocks, hid, weight, residual, post_gain, final_gain, targets, vocab, bias):
    count, rows, _ = hid.shape
    width = weight.shape[1]
    split_rows = rows // splits
    dma = pltpu.SemaphoreType.DMA
    vmem = pl.BlockSpec(memory_space=pltpu.VMEM)
    hbm = pl.BlockSpec(memory_space=pl.ANY)
    cols, lanes = bias.shape[1], targets.shape[1]
    flops = 2 * count * rows * weight.shape[0] * width
    return pl.pallas_call(
        functools.partial(front_kernel, nx, nz, splits, blocks),
        out_shape=(
            *[jax.ShapeDtypeStruct((2, count, splits, split_rows, width // blocks), bf16)] * blocks,
            jax.ShapeDtypeStruct((2, count, rows, cols), bf16),
            jax.ShapeDtypeStruct((splits, split_rows, width), bf16),
            jax.ShapeDtypeStruct((1, lanes), f32),
        ),
        in_specs=[hbm] * 2 + [vmem] * 4 + [hbm, vmem],
        out_specs=(*[hbm] * blocks, hbm, vmem, vmem),
        scratch_shapes=[pltpu.VMEM(hid.shape, bf16), pltpu.VMEM(weight.shape, bf16)]
        + rs_scratch(nx, nz, splits, split_rows, width)
        + [
            pltpu.VMEM((2, count, splits, split_rows, width), bf16),
            pltpu.VMEM((2, count, 1, lanes), jnp.int32),
            pltpu.VMEM((width, cols), bf16),
            pltpu.VMEM((2 * rows, cols), f32),
            pltpu.VMEM((2, count, rows, cols), bf16),
            pltpu.VMEM((2, count, 8, lanes), f32),
            pltpu.VMEM((2, count, 8, lanes), f32),
            pltpu.VMEM((1, lanes), f32),
            pltpu.VMEM((2, count, 1, lanes), f32),
        ]
        + rs_sems(nx, nz, splits)
        + [
            dma((count - 1,)), dma((count,)), dma((2, count)), dma((2, count)),
            dma((nx - 1, nz, splits)), dma((2, nz, splits)), dma((count, splits)),
            dma((count, splits)), dma((count, splits)), dma((2, count, splits)),
            dma, dma, dma((2, count)), dma((2, count)), dma((2, count)), dma((2, count)),
            dma((2, count)),
        ],
        compiler_params=pltpu.CompilerParams(
            collective_id=0, has_side_effects=True, vmem_limit_bytes=60 << 20
        ),
        cost_estimate=pl.CostEstimate(flops=flops, bytes_accessed=1 << 24, transcendentals=0),
        name="front",
    )(hid, weight, residual.reshape(splits, split_rows, width), post_gain, final_gain, targets,
      vocab, bias)


def back_kernel(
    nx, nz, splits,
    dlogits, vocab, kept_rows, given_rows, own_out, kept_out, cross_out,
    grads, vocab_part, token_rows, turned, kept, cross, terms, given, theirs, px, xr, q, sb, zd, zu,
    xs_sem, xr_sem, zs_sem, zd_sem, zu_sem,
    load_sem, vocab_sem, core_send, core_recv,
    rows_sem, kept_sem, cross_send, cross_recv,
):
    place = Place(nx, nz)
    count, z = place.count, place.z
    split_rows = q.shape[2]
    rows = splits * split_rows
    cols = vocab_part.shape[2]
    pieces, piece = vocab_part.shape[0], vocab_part.shape[1]
    core = lax.rem(place.dp, 2)
    greet(place, False)

    def load(zb):
        for step in range(nx):
            i = zb * nx + place.side(step)
            for c in range(2):
                pltpu.make_async_copy(dlogits.at[c, i], grads.at[c, i], load_sem.at[c, i]).start()

    load(0)
    for n in range(pieces):
        pltpu.make_async_copy(
            vocab.at[n * piece : (n + 1) * piece, pl.ds(pl.multiple_of(core * cols, cols), cols)],
            vocab_part.at[n], vocab_sem.at[n],
        ).start()

    @pl.loop(1, nz)
    def _(k):
        load(place.outward(k))

    for b, ref in enumerate((kept_rows, given_rows)):
        pltpu.make_async_copy(ref, token_rows.at[b], rows_sem.at[b]).start()

    tokens, _ = token_rows.shape[1:]
    slab = min(tokens, 256)
    span = kept.shape[2]

    def turn():
        @pl.loop(1, nz)
        def _(k):
            for step in range(nx):
                i = place.outward(k) * nx + place.side(step)
                for c in range(2):
                    arrived(grads.at[c, i], load_sem.at[c, i])

        for b in range(2):
            arrived(token_rows.at[b], rows_sem.at[b])

            @pl.loop(0, tokens // slab)
            def _(n):
                at = pl.ds(pl.multiple_of(n * slab, slab), slab)
                turned[b, :, at] = jnp.transpose(token_rows[b, at, :])

    def own_gradient(k):
        at = pl.ds(pl.multiple_of(k * span, span), span)
        part = grads[:, :, :, at].reshape(tokens, span)
        kept[k] = jnp.dot(turned[0], part, preferred_element_type=f32)
        cross[k] = jnp.dot(turned[1], part, preferred_element_type=f32).astype(bf16)
        pltpu.make_async_copy(kept.at[k], kept_out.at[:, at], kept_sem.at[k]).start()
        send(cross.at[k], cross_out.at[:, at], cross_send.at[k], cross_recv.at[k],
             (place.vp, place.other_core))

    def produce(zb):
        for step in range(nx):
            i = zb * nx + place.side(step)

            @pl.when(zb == 0)
            def _():
                for c in range(2):
                    arrived(grads.at[c, i], load_sem.at[c, i])

            block = jnp.concatenate([grads[0, i], grads[1, i]], axis=0)

            @pl.loop(0, pieces)
            def _(n):
                if step == 0:
                    @pl.when(zb == 0)
                    def _():
                        arrived(vocab_part.at[n], vocab_sem.at[n])

                at = pl.ds(pl.multiple_of(n * piece, piece), piece)
                value = lax.dot_general(
                    block, vocab_part[n], (((1,), (1,)), ((), ())), preferred_element_type=f32
                )
                for s in range(splits):
                    r = s * split_rows
                    terms[step, s, :, at] = value[r : r + split_rows]
                    given[i, s, :, at] = value[rows + r : rows + r + split_rows].astype(bf16)

            for s in range(splits):
                send(given.at[i, s], theirs.at[i, s], core_send.at[i, s], core_recv.at[i, s],
                     (place.vp, place.other_core))
        for step in range(nx):
            i = zb * nx + place.side(step)
            for s in range(splits):
                arrived(theirs.at[i, s], core_recv.at[i, s])

                def body(r):
                    value = terms[step, s, r] + theirs[i, s, r].astype(f32)
                    if step == 0:
                        q[zb, s, r] = value
                    else:
                        px[step - 1, zb, s, r] = value.astype(bf16)

                row_loop(split_rows, 16, body)

    count_own = kept.shape[0]

    early = count_own // 2

    def meanwhile(k):
        if k is None:
            pl.loop(early, count_own)(own_gradient)
            return

        @pl.when(k == 0)
        def _():
            turn()

        if early > 0:
            @pl.when(k == nz)
            def _():
                pl.loop(0, early)(own_gradient)

    line_reduce_scatter(
        place, splits, produce, px, xr, q, sb, zd, zu, (xs_sem, xr_sem, zs_sem, zd_sem, zu_sem),
        meanwhile,
    )
    for s in range(splits):
        def body(r):
            own_out[s, r] = q[z, s, r]

        row_loop(split_rows, 16, body)

    @pl.loop(0, kept.shape[0])
    def _(k):
        arrived(kept.at[k], kept_sem.at[k])
        arrived(cross.at[k], cross_send.at[k])
        arrived(cross.at[k], cross_recv.at[k])

    @pl.loop(0, count)
    def _(i):
        for s in range(splits):
            arrived(given.at[i, s], core_send.at[i, s])


def back(nx, nz, splits, dlogits, vocab, kept_rows, given_rows):
    _, count, rows, cols = dlogits.shape
    width = vocab.shape[0]
    split_rows = rows // splits
    piece = math.gcd(width, 512)
    tokens, block = kept_rows.shape
    steps = max(1, min(nz, cols // 512))
    dma = pltpu.SemaphoreType.DMA
    shape = (count, splits, split_rows, width)
    hbm = pl.BlockSpec(memory_space=pl.ANY)
    return pl.pallas_call(
        functools.partial(back_kernel, nx, nz, splits),
        out_shape=(
            jax.ShapeDtypeStruct((splits, split_rows, width), f32),
            jax.ShapeDtypeStruct((block, cols), f32),
            jax.ShapeDtypeStruct((block, cols), bf16),
        ),
        in_specs=[hbm] * 4,
        out_specs=(pl.BlockSpec(memory_space=pltpu.VMEM), hbm, hbm),
        scratch_shapes=[
            pltpu.VMEM((2, count, rows, cols), bf16),
            pltpu.VMEM((width // piece, piece, cols), bf16),
            pltpu.VMEM((2, tokens, block), bf16),
            pltpu.VMEM((2, block, tokens), bf16),
            pltpu.VMEM((steps, block, cols // steps), f32),
            pltpu.VMEM((steps, block, cols // steps), bf16),
            pltpu.VMEM((nx, splits, split_rows, width), f32),
            pltpu.VMEM(shape, bf16),
            pltpu.VMEM(shape, bf16),
        ]
        + rs_scratch(nx, nz, splits, split_rows, width)
        + rs_sems(nx, nz, splits)
        + [dma((2, count)), dma((width // piece,)), dma((count, splits)), dma((count, splits))]
        + [dma((2,)), dma((steps,)), dma((steps,)), dma((steps,))],
        compiler_params=pltpu.CompilerParams(
            collective_id=1, has_side_effects=True, vmem_limit_bytes=62 << 20
        ),
        cost_estimate=pl.CostEstimate(
            flops=4 * count * rows * cols * width, bytes_accessed=1 << 24, transcendentals=0
        ),
        name="back",
    )(dlogits, vocab, kept_rows, given_rows)


def on_device(
    nx, nz, hidden, down_weight, residual, post_gain, final_gain, vocab_matrix, vocab_bias, targets
):
    rows, width = residual.shape
    count = lax.axis_size("vp")
    dp_size = lax.axis_size("dp")
    planes = dp_size // 2
    splits = 4 if rows % 64 == 0 else 2 if rows % 32 == 0 else 1
    core = lax.axis_index("dp") % 2
    units = hidden.reshape(rows, count, hidden.shape[1] // count).transpose(1, 0, 2)
    lanes = -(-rows // 128) * 128
    padded = jnp.pad(targets, (0, lanes - rows)).reshape(1, lanes)
    cols = vocab_matrix.shape[1] // 2
    bias_half = lax.dynamic_slice_in_dim(vocab_bias, core * cols, cols, 0)
    *normed, dlogits, stream, losses = front(
        nx, nz, splits, 2 * planes, units, down_weight, residual,
        post_gain.reshape(1, -1), final_gain.reshape(1, -1), padded,
        vocab_matrix, bias_half.reshape(1, -1),
    )
    stream = stream.reshape(rows, width)
    tokens = 2 * count * rows
    block = width // (2 * planes)
    token_rows = [part.reshape(tokens, block) for part in normed]
    dlogits_2d = dlogits.reshape(tokens, cols)

    spans = column_spans(cols)
    arrivals = []
    source = dlogits_2d
    for low, high in spans:
        got = []
        for shift in range(1, planes):
            for c in range(2):
                grads = lax.dot_general(
                    token_rows[2 * shift + c], source[:, low:high],
                    (((0,), (0,)), ((), ())), preferred_element_type=f32,
                ).astype(bf16)
                grads, source = lax.optimization_barrier((grads, source))
                to = [
                    (d, ((d // 2 + shift) % planes) * 2 + (d % 2 + c) % 2) for d in range(dp_size)
                ]
                got.append(lax.ppermute(grads, "dp", to))
        arrivals.append(got)
    dnormed, kept, given = back(
        nx, nz, splits, source.reshape(dlogits.shape), vocab_matrix,
        token_rows[0], token_rows[1],
    )
    dnormed = dnormed.reshape(rows, width)

    def total(c, base):
        parts = [
            sum(arrivals[k][2 * j + c].astype(f32) for j in range(planes - 1))
            for k in range(len(spans))
        ]
        return base.astype(f32) + jnp.concatenate(parts, axis=1)

    same, cross = total(0, kept), total(1, given)
    vocab_grad = jnp.concatenate(
        [jnp.where(core == 0, same, cross), jnp.where(core == 0, cross, same)], axis=1
    )
    stream_f = stream.astype(f32)
    inverse = lax.rsqrt(jnp.mean(stream_f * stream_f, axis=-1, keepdims=True) + norm_eps)
    scaled = stream_f * inverse
    dscaled = dnormed * final_gain[None, :]
    norm_grad = inverse * (dscaled - scaled * jnp.mean(dscaled * scaled, axis=-1, keepdims=True))
    return (losses[0, :rows], norm_grad, vocab_grad)


def column_spans(cols):
    first = 512
    return ((0, first), (first, cols)) if cols > first else ((0, cols),)


def solution(mesh):
    count = mesh.shape["vp"]
    nx = math.isqrt(count // 2)
    nx = nx if nx > 1 and count % nx == 0 else 2
    placed = (
        P(("vp", "dp"), None), P("vp", None), P(("vp", "dp"), None), P(), P(),
        P(None, "vp"), P("vp"), P(("vp", "dp")),
    )
    return jax.shard_map(
        functools.partial(on_device, nx, count // nx),
        mesh=mesh,
        in_specs=placed,
        out_specs=(P(("vp", "dp")), P(("vp", "dp"), None), P("dp", "vp")),
        check_vma=False,
    )
```
